32 devices in a mesh: sp: 8 (over z, core), tp: 4 (over y, x).
Axes of the slice: x: 2, y: 2, z: 4, core: 2. Of those that a mesh axis runs over, the one named last changes fastest.
Arguments:
- layer_input: bfloat16 [8192, 4096], P('sp', 'tp'), may hold values from -6 to 6
- key_weight: bfloat16 [4096, 4096], P(None, 'tp'), may hold values from -0.09375 to 0.09375
- value_weight: bfloat16 [4096, 4096], P(None, 'tp'), may hold values from -0.09375 to 0.09375
- decay_exponent: float32 [32], P('tp'), may hold values from -0.077 to -0.00016845703, as said below
- query_new: bfloat16 [2, 4096], P(None, 'tp'), may hold values from -6 to 6
- key_new: bfloat16 [2, 4096], P(None, 'tp'), may hold values from -6 to 6
- value_new: bfloat16 [2, 4096], P(None, 'tp'), may hold values from -6 to 6
- norm_gain: float32 [4096], P('tp'), may hold values from 0.1 to 1.9
Outputs:
- state_cache: bfloat16 [2, 32, 128, 128], P(None, 'tp', 'sp')
- first_read: bfloat16 [2, 4096], P(None, 'tp')
The draws below stay inside these ranges and needn't reach their ends.
Inputs may be any that keep to these rules, and one draw needn't show every extreme that they name: decay_exponent is negative.
All inputs are finite; a program needn't handle non-finite values.
Results may differ from the reference program's by a relative error of at most 0.011.
Values may be sent and summed in bfloat16 or wider, within the bound.
A program may use at most 64 MiB of HBM per device.

```python
import jax
import jax.numpy as jnp
from jax import lax

D = 4096
HEADS = 32
DK = 128
DV = 128
SEQS = 2
TOKENS = 8192
LEN = 4096


def draw_decay_exponent(key, part):
    first_key = jax.random.fold_in(key, 11)
    second_key = jax.random.fold_in(key, 12)
    third_key = jax.random.fold_in(key, 13)
    slow_share = 0.5
    slow_flag = jax.random.uniform(first_key, (HEADS,), jnp.float32) < slow_share
    fast_rate = jax.random.uniform(second_key, (HEADS,), jnp.float32, 2.3026 / 100.0, 2.3026 / 30.0)
    slow_rate = jax.random.uniform(third_key, (HEADS,), jnp.float32, 0.3, 1.0) * (2.3026 / LEN)
    return -jnp.where(slow_flag, slow_rate, fast_rate)


def levels(rng, dims, shards, least, largest):
    def one(dim, parts):
        draws = jax.random.uniform(jax.random.fold_in(jax.random.fold_in(rng, 6), dim), (parts,), jnp.float32, least / len(shards), largest / len(shards))
        return jnp.repeat(jnp.exp(draws), dims[dim] // parts).reshape((-1,) + (1,) * (len(dims) - dim - 1))

    gain = one(*shards[0])
    for cut in shards[1:]:
        gain = gain * one(*cut)
    return gain


def bell_draw(stream_key, extent, spread, most, split=(), kind=jnp.bfloat16):
    result = spread * jax.random.normal(stream_key, extent, jnp.float32)
    if split:
        result = result * levels(stream_key, extent, split, -0.22, 0.18)
    return jnp.clip(result, -most, most).astype(kind)


def setup_inputs(seed: int = 0) -> dict:
    key_of = jax.random.split(jax.random.key(seed), 9)
    return {
        "layer_input": bell_draw(key_of[0], (TOKENS, D), 1.0, 6.0, ((0, 8), (1, 4))),
        "key_weight": bell_draw(key_of[1], (D, HEADS * DK), D ** -0.5, 0.09375, ((1, 4),)),
        "value_weight": bell_draw(key_of[2], (D, HEADS * DV), D ** -0.5, 0.09375, ((1, 4),)),
        "decay_exponent": draw_decay_exponent(jax.random.fold_in(key_of[8], 71), 0),
        "query_new": bell_draw(key_of[4], (SEQS, HEADS * DK), 1.0, 6.0, ((1, 4),)),
        "key_new": bell_draw(key_of[5], (SEQS, HEADS * DK), 1.0, 6.0, ((1, 4),)),
        "value_new": bell_draw(key_of[6], (SEQS, HEADS * DV), 1.0, 6.0, ((1, 4),)),
        "norm_gain": jnp.clip(1.0 + 0.18 * jax.random.normal(key_of[7], (HEADS * DV,), jnp.float32), 0.1, 1.9),
    }


def rotate(projected, position):
    half_width = projected.shape[-1] // 2
    inverse = 1.0 / 10000.0 ** jnp.linspace(0.0, 1.0, half_width, dtype=jnp.float32)
    angle = position[:, None] * inverse[None, :]
    cosine = jnp.cos(angle)[:, None, :]
    sine = jnp.sin(angle)[:, None, :]
    first = projected[..., :half_width]
    second = projected[..., half_width:]
    return jnp.concatenate([first * cosine - second * sine, first * sine + second * cosine], axis=-1)

def reference(layer_input, key_weight, value_weight, decay_exponent, query_new, key_new, value_new, norm_gain):
    key_proj = jnp.dot(layer_input, key_weight, preferred_element_type=jnp.float32)
    value_proj = jnp.dot(layer_input, value_weight, preferred_element_type=jnp.float32)
    position = (jnp.arange(TOKENS, dtype=jnp.int32) % LEN).astype(jnp.float32)
    keys = (rotate(key_proj.reshape(TOKENS, HEADS, DK), position) * DK ** (-0.5)).astype(jnp.bfloat16)
    values = value_proj.astype(jnp.bfloat16).reshape(TOKENS, HEADS, DV)
    distance = LEN - 1.0 - position
    weighting = jnp.exp(decay_exponent[None, :] * distance[:, None])
    weighted = (keys.astype(jnp.float32) * weighting[:, :, None]).astype(jnp.bfloat16)
    final = jnp.einsum('slhd,slhe->shde', weighted.astype(jnp.float32).reshape(SEQS, LEN, HEADS, DK), values.astype(jnp.float32).reshape(SEQS, LEN, HEADS, DV), precision=lax.Precision.HIGHEST)
    state_cache = final.astype(jnp.bfloat16)
    queries = query_new.astype(jnp.float32).reshape(SEQS, HEADS, DK)
    keys_next = key_new.astype(jnp.float32).reshape(SEQS, HEADS, DK)
    values_next = value_new.astype(jnp.float32).reshape(SEQS, HEADS, DV)
    carried = jnp.einsum('shd,shde->she', queries, final, precision=lax.Precision.HIGHEST)
    own_term = lax.optimization_barrier(jnp.sum(queries * keys_next, axis=2))[:, :, None] * values_next
    mixed = jnp.exp(decay_exponent)[None, :, None] * carried + own_term
    normed = mixed * lax.rsqrt(lax.optimization_barrier(jnp.mean(mixed * mixed, axis=2, keepdims=True)) + 1e-06)
    normed = normed * norm_gain.reshape(HEADS, DV)[None, :, :]
    return (state_cache, normed.reshape(SEQS, HEADS * DV).astype(jnp.bfloat16))
```

```python
import functools
import math

import jax
import jax.numpy as jnp
import numpy as np
from jax import lax
from jax.experimental import pallas as pl
from jax.experimental.pallas import tpu as pltpu
from jax.sharding import PartitionSpec as P

SEQS = 2
CHUNKS = 4
MESH = pl.DeviceIdType.MESH
F32 = jnp.float32
BF16 = jnp.bfloat16


def gather_kernel(
    side, seq_span, chunks,
    decay_ref, inv_ref, x_ref, wk_ref, wv_ref,
    state_ref,
    gx, wk, wv, cosine, sine, acc_k, acc_v,
    send_sem, recv_sem, local_sem,
):
    tokens, feats = x_ref.shape
    rows = tokens // chunks
    half = rows // 2
    heads, width, vwidth = state_ref.shape
    pair = 2 if heads % 2 == 0 else 1
    me = lax.axis_index("tp")
    my_y, my_x = me // side, lax.rem(me, side)
    sp_place = lax.axis_index("sp")

    def x_peer(d):
        return my_y * side + lax.rem(my_x + d, side)

    def y_peer(d):
        return lax.rem(my_y + d, side) * side + my_x

    x_peers = [x_peer(d) for d in range(1, side)]
    y_peers = [y_peer(d) for d in range(1, side)]

    local = [
        pltpu.make_async_copy(x_ref, gx.at[me], local_sem.at[0]),
        pltpu.make_async_copy(wk_ref, wk, local_sem.at[1]),
        pltpu.make_async_copy(wv_ref, wv, local_sem.at[2]),
    ]
    for copy in local:
        copy.start()

    barrier = pltpu.get_barrier_semaphore()
    for peer in x_peers + y_peers:
        pl.semaphore_signal(barrier, inc=1, device_id={"tp": peer}, device_id_type=MESH)
    pl.semaphore_wait(barrier, 2 * (side - 1))

    def span(c, part):
        return pl.ds(pl.multiple_of(c * rows + part * half, half), half)

    def remote(c, slot, block, part, target, from_input):
        where = span(c, part)
        return pltpu.make_async_remote_copy(
            src_ref=x_ref.at[where] if from_input else gx.at[block, where],
            dst_ref=gx.at[block, where],
            send_sem=send_sem.at[c, slot],
            recv_sem=recv_sem.at[c, block, part],
            device_id={"tp": target},
            device_id_type=MESH,
        )

    def own_copies(c):
        out, slot = [], 0
        for first in (True, False):
            for part, peers in ((0, x_peers), (1, y_peers)):
                for peer in peers:
                    out.append(remote(c, slot, me, part if first else 1 - part, peer, True))
                    slot += 1
        return out

    def relay_copies(c):
        out, slot = [], 4 * (side - 1)
        for part, sources, peers in ((0, x_peers, y_peers), (1, y_peers, x_peers)):
            for source in sources:
                for peer in peers:
                    out.append(remote(c, slot, source, part, peer, False))
                    slot += 1
        return out

    def arrived(c, block, part):
        remote(c, 0, block, part, x_peers[0], False).wait_recv()

    late_blocks = [
        lax.rem(my_y + dy, side) * side + lax.rem(my_x + dx, side)
        for dy in range(1, side)
        for dx in range(1, side)
    ]

    def wait_early(c):
        for block in x_peers + y_peers:
            for part in range(2):
                arrived(c, block, part)

    def wait_late(c):
        for block in late_blocks:
            for part in range(2):
                arrived(c, block, part)

    def start_all(copies):
        for copy in copies:
            copy.start()

    start_all(own_copies(0))
    if chunks > 1:
        start_all(own_copies(1))

    state_ref[...] = jnp.zeros_like(state_ref)
    base = lax.rem(sp_place, seq_span) * tokens

    def table(c, _):
        at = pl.ds(pl.multiple_of(c * half, half), half)
        place = (base + c * half + lax.broadcasted_iota(jnp.int32, (half, width), 0)).astype(F32)
        angle = place * inv_ref[...]
        low = lax.broadcasted_iota(jnp.int32, (half, width), 1) < width // 2
        sin = jnp.sin(angle)
        cosine[at, :] = jnp.cos(angle)
        sine[at, :] = jnp.where(low, -sin, sin)
        return 0

    lax.fori_loop(0, 2 * chunks, table, 0)
    for copy in local:
        copy.wait()

    def partial(c, blocks, w, cols):
        at = pl.ds(pl.multiple_of(c * rows, rows), rows)
        total = None
        for block in blocks:
            depth = pl.ds(pl.multiple_of(block * feats, feats), feats)
            term = jnp.dot(gx[block, at, :], w[depth, cols], preferred_element_type=F32)
            total = term if total is None else total + term
        return total

    early_blocks = [me] + x_peers + y_peers

    def finish(c, blocks, carry):
        at = pl.ds(pl.multiple_of(c * rows, rows), rows)
        distance = (seq_span * tokens - 1 - base - c * rows) - lax.broadcasted_iota(
            jnp.int32, (rows, width), 0
        )
        distance = distance.astype(F32)

        def step(g, _):
            kcols = pl.ds(pl.multiple_of(g * pair * width, pair * width), pair * width)
            vcols = pl.ds(pl.multiple_of(g * pair * vwidth, pair * vwidth), pair * vwidth)
            k = partial(c, blocks, wk, kcols)
            v = partial(c, blocks, wv, vcols)
            if carry:
                k = k + acc_k[:, kcols]
                v = v + acc_v[:, vcols]
            v = v.astype(BF16)
            for j in range(pair):
                kh = k[:, j * width:(j + 1) * width]
                turned = kh * cosine[at, :] + pltpu.roll(kh, width // 2, 1) * sine[at, :]
                keys = (turned * width ** (-0.5)).astype(BF16).astype(F32)
                weighted = (keys * jnp.exp(decay_ref[g * pair + j] * distance)).astype(BF16)
                state_ref[g * pair + j] += lax.dot_general(
                    weighted, v[:, j * vwidth:(j + 1) * vwidth],
                    (((0,), (0,)), ((), ())), preferred_element_type=F32,
                )
            return 0

        lax.fori_loop(0, heads // pair, step, 0)

    def round_trip(c, _):
        wait_early(c)
        start_all(relay_copies(c))

        @pl.when(c + 2 < chunks)
        def _():
            start_all(own_copies(c + 2))

        @pl.when(c > 0)
        def _():
            wait_late(c - 1)
            finish(c - 1, early_blocks + late_blocks, False)

        return 0

    lax.fori_loop(0, chunks, round_trip, 0)
    last = chunks - 1

    def early(g, _):
        kcols = pl.ds(pl.multiple_of(g * pair * width, pair * width), pair * width)
        vcols = pl.ds(pl.multiple_of(g * pair * vwidth, pair * vwidth), pair * vwidth)
        acc_k[:, kcols] = partial(last, early_blocks, wk, kcols)
        acc_v[:, vcols] = partial(last, early_blocks, wv, vcols)
        return 0

    lax.fori_loop(0, heads // pair, early, 0)
    wait_late(last)
    finish(last, late_blocks, True)

    def drain(c, _):
        for copy in own_copies(c) + relay_copies(c):
            copy.wait_send()
        return 0

    lax.fori_loop(0, chunks, drain, 0)


def local_states(layer_input, key_weight, value_weight, decay_exponent, seq_span):
    tokens, feats = layer_input.shape
    depth = key_weight.shape[0]
    parts = lax.axis_size("tp")
    side = math.isqrt(parts)
    heads = decay_exponent.shape[0]
    width = key_weight.shape[1] // heads
    vwidth = value_weight.shape[1] // heads
    steps = np.linspace(0.0, 1.0, width // 2, dtype=np.float32)
    inverse = (np.float32(1.0) / np.power(np.float32(10000.0), steps)).astype(np.float32)
    inverse = jnp.asarray(np.concatenate([inverse, inverse])[None, :])
    sends = 4 * (side - 1) + 2 * (side - 1) ** 2
    anywhere = pl.BlockSpec(memory_space=pl.ANY)
    vmem = pl.BlockSpec(memory_space=pltpu.VMEM)
    rows = tokens // CHUNKS
    return pl.pallas_call(
        functools.partial(gather_kernel, side, seq_span, CHUNKS),
        out_shape=jax.ShapeDtypeStruct((heads, width, vwidth), F32),
        in_specs=[pl.BlockSpec(memory_space=pltpu.SMEM), vmem, anywhere, anywhere, anywhere],
        out_specs=vmem,
        scratch_shapes=[
            pltpu.VMEM((parts, tokens, feats), BF16),
            pltpu.VMEM(key_weight.shape, BF16),
            pltpu.VMEM(value_weight.shape, BF16),
            pltpu.VMEM((tokens, width), F32),
            pltpu.VMEM((tokens, width), F32),
            pltpu.VMEM((rows, heads * width), F32),
            pltpu.VMEM((rows, heads * vwidth), F32),
            pltpu.SemaphoreType.DMA((CHUNKS, sends)),
            pltpu.SemaphoreType.DMA((CHUNKS, parts, 2)),
            pltpu.SemaphoreType.DMA((3,)),
        ],
        compiler_params=pltpu.CompilerParams(
            collective_id=0, has_side_effects=True, vmem_limit_bytes=56 * 1024 * 1024
        ),
    )(decay_exponent, inverse, layer_input, key_weight, value_weight)


def on_device(
    layer_input, key_weight, value_weight, decay_exponent, query_new, key_new, value_new, norm_gain
):
    head_local = decay_exponent.shape[0]
    key_width = key_weight.shape[1] // head_local
    value_width = value_weight.shape[1] // head_local
    seq_span = lax.axis_size("sp") // SEQS
    sp_place = lax.axis_index("sp")
    local_state = local_states(layer_input, key_weight, value_weight, decay_exponent, seq_span)
    member = (jnp.arange(SEQS, dtype=jnp.int32) == sp_place // seq_span).astype(jnp.float32)
    state_terms = member[:, None, None, None] * local_state[None]
    final_rows = lax.psum_scatter(state_terms, "sp", scatter_dimension=2, tiled=True)
    state_cache = final_rows.astype(jnp.bfloat16)
    queries = query_new.astype(jnp.float32).reshape(SEQS, head_local, key_width)
    partial_read = jnp.einsum(
        "shd,shde->she", queries, state_terms, precision=lax.Precision.HIGHEST
    )
    carried = lax.psum(partial_read, "sp")
    keys_next = key_new.astype(jnp.float32).reshape(SEQS, head_local, key_width)
    values_next = value_new.astype(jnp.float32).reshape(SEQS, head_local, value_width)
    own_term = jnp.sum(queries * keys_next, axis=2)[:, :, None] * values_next
    mixed = jnp.exp(decay_exponent)[None, :, None] * carried + own_term
    normed = mixed * lax.rsqrt(jnp.mean(mixed * mixed, axis=2, keepdims=True) + 1e-06)
    normed = normed * norm_gain.reshape(head_local, value_width)[None, :, :]
    return (state_cache, normed.reshape(SEQS, head_local * value_width).astype(jnp.bfloat16))


def solution(mesh):
    in_specs = (
        P("sp", "tp"),
        P(None, "tp"),
        P(None, "tp"),
        P("tp"),
        P(None, "tp"),
        P(None, "tp"),
        P(None, "tp"),
        P("tp"),
    )
    out_specs = (P(None, "tp", "sp", None), P(None, "tp"))
    return jax.shard_map(
        on_device, mesh=mesh, in_specs=in_specs, out_specs=out_specs, check_vma=False
    )
```

```python
import functools
import math

import jax
import jax.numpy as jnp
import numpy as np
from jax import lax
from jax.experimental import pallas as pl
from jax.experimental.pallas import tpu as pltpu
from jax.sharding import PartitionSpec as P

SEQS = 2
CHUNKS = 4
MESH = pl.DeviceIdType.MESH
F32 = jnp.float32
BF16 = jnp.bfloat16


def gather_kernel(
    side, seq_span, chunks,
    decay_ref, inv_ref, query_ref, key_ref, value_ref, gain_ref, x_ref, wk_ref, wv_ref,
    cache_ref, first_ref,
    gx, wk, wv, cosine, sine, acc_k, acc_v,
    state_ref, query_wide, own_term, factor, staged, landed, read, reads,
    send_sem, recv_sem, local_sem, state_send, state_recv, read_send, read_recv,
):
    tokens, feats = x_ref.shape
    rows = tokens // chunks
    half = rows // 2
    heads, width, vwidth = state_ref.shape
    pair = 2 if heads % 2 == 0 else 1
    me = lax.axis_index("tp")
    my_y, my_x = me // side, lax.rem(me, side)
    sp_place = lax.axis_index("sp")
    sp_size = landed.shape[0]
    kept = landed.shape[2]
    groups = heads // pair
    sp_peers = [lax.rem(sp_place + d, sp_size) for d in range(1, sp_size)]

    def x_peer(d):
        return my_y * side + lax.rem(my_x + d, side)

    def y_peer(d):
        return lax.rem(my_y + d, side) * side + my_x

    x_peers = [x_peer(d) for d in range(1, side)]
    y_peers = [y_peer(d) for d in range(1, side)]

    local = [
        pltpu.make_async_copy(x_ref, gx.at[me], local_sem.at[0]),
        pltpu.make_async_copy(wk_ref, wk, local_sem.at[1]),
        pltpu.make_async_copy(wv_ref, wv, local_sem.at[2]),
    ]
    for copy in local:
        copy.start()

    barrier = pltpu.get_barrier_semaphore()
    for peer in x_peers + y_peers:
        pl.semaphore_signal(barrier, inc=1, device_id={"tp": peer}, device_id_type=MESH)
    for peer in sp_peers:
        pl.semaphore_signal(barrier, inc=1, device_id={"sp": peer}, device_id_type=MESH)
    pl.semaphore_wait(barrier, 2 * (side - 1) + sp_size - 1)

    def span(c, part):
        return pl.ds(pl.multiple_of(c * rows + part * half, half), half)

    def remote(c, slot, block, part, target, from_input):
        where = span(c, part)
        return pltpu.make_async_remote_copy(
            src_ref=x_ref.at[where] if from_input else gx.at[block, where],
            dst_ref=gx.at[block, where],
            send_sem=send_sem.at[c, slot],
            recv_sem=recv_sem.at[c, block, part],
            device_id={"tp": target},
            device_id_type=MESH,
        )

    def own_copies(c):
        out, slot = [], 0
        for first in (True, False):
            for part, peers in ((0, x_peers), (1, y_peers)):
                for peer in peers:
                    out.append(remote(c, slot, me, part if first else 1 - part, peer, True))
                    slot += 1
        return out

    def relay_copies(c):
        out, slot = [], 4 * (side - 1)
        for part, sources, peers in ((0, x_peers, y_peers), (1, y_peers, x_peers)):
            for source in sources:
                for peer in peers:
                    out.append(remote(c, slot, source, part, peer, False))
                    slot += 1
        return out

    def arrived(c, block, part):
        remote(c, 0, block, part, x_peers[0], False).wait_recv()

    late_blocks = [
        lax.rem(my_y + dy, side) * side + lax.rem(my_x + dx, side)
        for dy in range(1, side)
        for dx in range(1, side)
    ]

    def wait_early(c):
        for block in x_peers + y_peers:
            for part in range(2):
                arrived(c, block, part)

    def wait_late(c):
        for block in late_blocks:
            for part in range(2):
                arrived(c, block, part)

    def start_all(copies):
        for copy in copies:
            copy.start()

    start_all(own_copies(0))
    if chunks > 1:
        start_all(own_copies(1))

    state_ref[...] = jnp.zeros_like(state_ref)
    base = lax.rem(sp_place, seq_span) * tokens

    def table(c, _):
        at = pl.ds(pl.multiple_of(c * half, half), half)
        place = (base + c * half + lax.broadcasted_iota(jnp.int32, (half, width), 0)).astype(F32)
        angle = place * inv_ref[...]
        low = lax.broadcasted_iota(jnp.int32, (half, width), 1) < width // 2
        sin = jnp.sin(angle)
        cosine[at, :] = jnp.cos(angle)
        sine[at, :] = jnp.where(low, -sin, sin)
        return 0

    lax.fori_loop(0, 2 * chunks, table, 0)

    prompt = sp_place // seq_span
    diagonal = lax.broadcasted_iota(jnp.int32, (width, width), 0) == lax.broadcasted_iota(
        jnp.int32, (width, width), 1
    )
    ones = jnp.ones((width, vwidth), BF16)
    queries = query_ref[...].astype(F32)
    next_keys = key_ref[...].astype(F32)
    next_values = value_ref[...].astype(F32)
    for h in range(heads):
        cols = slice(h * width, (h + 1) * width)
        vcols = slice(h * vwidth, (h + 1) * vwidth)
        mine = jnp.zeros((1, width), F32)
        for s in range(SEQS):
            mine = jnp.where(prompt == s, queries[s:s + 1, cols], mine)
            score = jnp.sum(
                queries[s:s + 1, cols] * next_keys[s:s + 1, cols], axis=1, keepdims=True
            )
            own_term[s, h] = score * next_values[s:s + 1, vcols]
        spread = jnp.where(diagonal, jnp.broadcast_to(mine, (width, width)), 0.0).astype(BF16)
        query_wide[h] = jnp.dot(spread, ones, preferred_element_type=F32)
        factor[h] = jnp.exp(jnp.full((1, vwidth), decay_ref[h], F32))

    def state_copies(g):
        piece = pl.ds(g * pair, pair)
        return [
            pltpu.make_async_remote_copy(
                src_ref=staged.at[peer, piece],
                dst_ref=landed.at[sp_place, piece],
                send_sem=state_send.at[g, d],
                recv_sem=state_recv.at[g, sp_place],
                device_id={"sp": peer},
                device_id_type=MESH,
            )
            for d, peer in enumerate(sp_peers)
        ]

    def read_copies():
        return [
            pltpu.make_async_remote_copy(
                src_ref=read,
                dst_ref=reads.at[sp_place],
                send_sem=read_send.at[d],
                recv_sem=read_recv.at[sp_place],
                device_id={"sp": peer},
                device_id_type=MESH,
            )
            for d, peer in enumerate(sp_peers)
        ]

    for copy in local:
        copy.wait()

    def partial(c, blocks, w, cols):
        at = pl.ds(pl.multiple_of(c * rows, rows), rows)
        total = None
        for block in blocks:
            depth = pl.ds(pl.multiple_of(block * feats, feats), feats)
            term = jnp.dot(gx[block, at, :], w[depth, cols], preferred_element_type=F32)
            total = term if total is None else total + term
        return total

    early_blocks = [me] + x_peers + y_peers

    def finish(c, blocks, carry):
        at = pl.ds(pl.multiple_of(c * rows, rows), rows)
        distance = (seq_span * tokens - 1 - base - c * rows) - lax.broadcasted_iota(
            jnp.int32, (rows, width), 0
        )
        distance = distance.astype(F32)

        def step(g, _):
            kcols = pl.ds(pl.multiple_of(g * pair * width, pair * width), pair * width)
            vcols = pl.ds(pl.multiple_of(g * pair * vwidth, pair * vwidth), pair * vwidth)
            k = partial(c, blocks, wk, kcols)
            v = partial(c, blocks, wv, vcols)
            if carry:
                k = k + acc_k[:, kcols]
                v = v + acc_v[:, vcols]
            v = v.astype(BF16)
            for j in range(pair):
                kh = k[:, j * width:(j + 1) * width]
                turned = kh * cosine[at, :] + pltpu.roll(kh, width // 2, 1) * sine[at, :]
                keys = (turned * width ** (-0.5)).astype(BF16).astype(F32)
                weighted = (keys * jnp.exp(decay_ref[g * pair + j] * distance)).astype(BF16)
                state_ref[g * pair + j] += lax.dot_general(
                    weighted, v[:, j * vwidth:(j + 1) * vwidth],
                    (((0,), (0,)), ((), ())), preferred_element_type=F32,
                )
            if carry:
                for j in range(pair):
                    h = g * pair + j
                    held = state_ref[h]
                    for d in range(sp_size):
                        staged[d, h] = held[d * kept:(d + 1) * kept, :].astype(BF16)
                    read[h] = jnp.sum(query_wide[h] * held, axis=0, keepdims=True)
                start_all(state_copies(g))
            return 0

        lax.fori_loop(0, groups, step, 0)

    def round_trip(c, _):
        wait_early(c)
        start_all(relay_copies(c))

        @pl.when(c + 2 < chunks)
        def _():
            start_all(own_copies(c + 2))

        @pl.when(c > 0)
        def _():
            wait_late(c - 1)
            finish(c - 1, early_blocks + late_blocks, False)

        return 0

    lax.fori_loop(0, chunks, round_trip, 0)
    last = chunks - 1

    def early(g, _):
        kcols = pl.ds(pl.multiple_of(g * pair * width, pair * width), pair * width)
        vcols = pl.ds(pl.multiple_of(g * pair * vwidth, pair * vwidth), pair * vwidth)
        acc_k[:, kcols] = partial(last, early_blocks, wk, kcols)
        acc_v[:, vcols] = partial(last, early_blocks, wv, vcols)
        return 0

    lax.fori_loop(0, heads // pair, early, 0)
    wait_late(last)
    finish(last, late_blocks, True)

    start_all(read_copies())
    landed[sp_place] = staged[sp_place]
    reads[sp_place] = read[...]

    for d, peer in enumerate(sp_peers):
        pltpu.make_async_remote_copy(
            src_ref=read, dst_ref=reads.at[peer], send_sem=read_send.at[d],
            recv_sem=read_recv.at[peer], device_id={"sp": peer}, device_id_type=MESH,
        ).wait_recv()
        for g in range(groups):
            piece = pl.ds(g * pair, pair)
            pltpu.make_async_remote_copy(
                src_ref=staged.at[peer, piece], dst_ref=landed.at[peer, piece],
                send_sem=state_send.at[g, d], recv_sem=state_recv.at[g, peer],
                device_id={"sp": peer}, device_id_type=MESH,
            ).wait_recv()

    row = lax.broadcasted_iota(jnp.int32, (SEQS, heads * vwidth), 0)
    out = jnp.zeros((SEQS, heads * vwidth), F32)
    for s in range(SEQS):
        members = range(s * seq_span, (s + 1) * seq_span)
        carried = functools.reduce(jnp.add, [reads[m] for m in members])
        mixed = factor[...] * carried + own_term[s]
        normed = mixed * lax.rsqrt(jnp.mean(mixed * mixed, axis=2, keepdims=True) + 1e-06)
        line = jnp.concatenate([normed[h] for h in range(heads)], axis=1) * gain_ref[...]
        out = jnp.where(row == s, jnp.broadcast_to(line, out.shape), out)
        for h in range(heads):
            cache_ref[s, h] = functools.reduce(
                jnp.add, [landed[m, h].astype(F32) for m in members]
            ).astype(BF16)
    first_ref[...] = out.astype(BF16)

    for copy in read_copies():
        copy.wait_send()
    for g in range(groups):
        for copy in state_copies(g):
            copy.wait_send()

    def drain(c, _):
        for copy in own_copies(c) + relay_copies(c):
            copy.wait_send()
        return 0

    lax.fori_loop(0, chunks, drain, 0)


def on_device(
    layer_input, key_weight, value_weight, decay_exponent, query_new, key_new, value_new, norm_gain
):
    tokens, feats = layer_input.shape
    parts = lax.axis_size("tp")
    sp_size = lax.axis_size("sp")
    seq_span = sp_size // SEQS
    side = math.isqrt(parts)
    heads = decay_exponent.shape[0]
    width = key_weight.shape[1] // heads
    vwidth = value_weight.shape[1] // heads
    kept = width // sp_size
    groups = heads // (2 if heads % 2 == 0 else 1)
    steps = np.linspace(0.0, 1.0, width // 2, dtype=np.float32)
    inverse = (np.float32(1.0) / np.power(np.float32(10000.0), steps)).astype(np.float32)
    inverse = jnp.asarray(np.concatenate([inverse, inverse])[None, :])
    sends = 4 * (side - 1) + 2 * (side - 1) ** 2
    anywhere = pl.BlockSpec(memory_space=pl.ANY)
    vmem = pl.BlockSpec(memory_space=pltpu.VMEM)
    rows = tokens // CHUNKS
    return pl.pallas_call(
        functools.partial(gather_kernel, side, seq_span, CHUNKS),
        out_shape=(
            jax.ShapeDtypeStruct((SEQS, heads, kept, vwidth), BF16),
            jax.ShapeDtypeStruct((SEQS, heads * vwidth), BF16),
        ),
        in_specs=[pl.BlockSpec(memory_space=pltpu.SMEM)] + [vmem] * 5 + [anywhere] * 3,
        out_specs=(vmem, vmem),
        scratch_shapes=[
            pltpu.VMEM((parts, tokens, feats), BF16),
            pltpu.VMEM(key_weight.shape, BF16),
            pltpu.VMEM(value_weight.shape, BF16),
            pltpu.VMEM((tokens, width), F32),
            pltpu.VMEM((tokens, width), F32),
            pltpu.VMEM((rows, heads * width), F32),
            pltpu.VMEM((rows, heads * vwidth), F32),
            pltpu.VMEM((heads, width, vwidth), F32),
            pltpu.VMEM((heads, width, vwidth), F32),
            pltpu.VMEM((SEQS, heads, 1, vwidth), F32),
            pltpu.VMEM((heads, 1, vwidth), F32),
            pltpu.VMEM((sp_size, heads, kept, vwidth), BF16),
            pltpu.VMEM((sp_size, heads, kept, vwidth), BF16),
            pltpu.VMEM((heads, 1, vwidth), F32),
            pltpu.VMEM((sp_size, heads, 1, vwidth), F32),
            pltpu.SemaphoreType.DMA((CHUNKS, sends)),
            pltpu.SemaphoreType.DMA((CHUNKS, parts, 2)),
            pltpu.SemaphoreType.DMA((3,)),
            pltpu.SemaphoreType.DMA((groups, sp_size - 1)),
            pltpu.SemaphoreType.DMA((groups, sp_size)),
            pltpu.SemaphoreType.DMA((sp_size - 1,)),
            pltpu.SemaphoreType.DMA((sp_size,)),
        ],
        compiler_params=pltpu.CompilerParams(
            collective_id=0, has_side_effects=True, vmem_limit_bytes=56 * 1024 * 1024
        ),
    )(
        decay_exponent, inverse, query_new, key_new, value_new, norm_gain.reshape(1, -1),
        layer_input, key_weight, value_weight,
    )


def solution(mesh):
    in_specs = (
        P("sp", "tp"),
        P(None, "tp"),
        P(None, "tp"),
        P("tp"),
        P(None, "tp"),
        P(None, "tp"),
        P(None, "tp"),
        P("tp"),
    )
    out_specs = (P(None, "tp", "sp", None), P(None, "tp"))
    return jax.shard_map(
        on_device, mesh=mesh, in_specs=in_specs, out_specs=out_specs, check_vma=False
    )
```

```python
import functools
import math

import jax
import jax.numpy as jnp
import numpy as np
from jax import lax
from jax.experimental import pallas as pl
from jax.experimental.pallas import tpu as pltpu
from jax.sharding import PartitionSpec as P

SEQS = 2
CHUNKS = 8
MESH = pl.DeviceIdType.MESH
F32 = jnp.float32
BF16 = jnp.bfloat16


def gather_kernel(
    side, seq_span, chunks,
    decay_hbm, inv_hbm, query_hbm, key_hbm, value_hbm, gain_hbm, x_ref, wk_ref, wv_ref,
    cache_ref, first_ref,
    decay_ref, inv_ref, query_ref, key_ref, value_ref, gain_ref,
    gx, wk, wv, cosine, sine, acc_k, acc_v,
    state_ref, query_wide, own_term, factor, staged, landed, read, reads,
    send_sem, recv_sem, local_sem, state_send, state_recv, read_send, read_recv,
):
    tokens, feats = x_ref.shape
    rows = tokens // chunks
    half = rows // 2
    heads, width, vwidth = state_ref.shape
    pair = 2 if heads % 2 == 0 else 1
    me = lax.axis_index("tp")
    my_y, my_x = me // side, lax.rem(me, side)
    sp_place = lax.axis_index("sp")
    sp_size = landed.shape[0]
    kept = landed.shape[2]
    groups = heads // pair
    sp_peers = [lax.rem(sp_place + d, sp_size) for d in range(1, sp_size)]

    def x_peer(d):
        return my_y * side + lax.rem(my_x + d, side)

    def y_peer(d):
        return lax.rem(my_y + d, side) * side + my_x

    x_peers = [x_peer(d) for d in range(1, side)]
    y_peers = [y_peer(d) for d in range(1, side)]

    barrier = pltpu.get_barrier_semaphore()
    for peer in x_peers + y_peers:
        pl.semaphore_signal(barrier, inc=1, device_id={"tp": peer}, device_id_type=MESH)
    for peer in sp_peers:
        pl.semaphore_signal(barrier, inc=1, device_id={"sp": peer}, device_id_type=MESH)
    pl.semaphore_wait(barrier, 2 * (side - 1) + sp_size - 1)

    def span(c, part):
        return pl.ds(pl.multiple_of(c * rows + part * half, half), half)

    def remote(c, slot, block, part, target, from_input):
        where = span(c, part)
        return pltpu.make_async_remote_copy(
            src_ref=x_ref.at[where] if from_input else gx.at[block, where],
            dst_ref=gx.at[block, where],
            send_sem=send_sem.at[c, slot],
            recv_sem=recv_sem.at[c, block, part],
            device_id={"tp": target},
            device_id_type=MESH,
        )

    def own_copies(c):
        out, slot = [], 0
        for first in (True, False):
            for part, peers in ((0, x_peers), (1, y_peers)):
                for peer in peers:
                    out.append(remote(c, slot, me, part if first else 1 - part, peer, True))
                    slot += 1
        return out

    def relay_copies(c):
        out, slot = [], 4 * (side - 1)
        for part, sources, peers in ((0, x_peers, y_peers), (1, y_peers, x_peers)):
            for source in sources:
                for peer in peers:
                    out.append(remote(c, slot, source, part, peer, False))
                    slot += 1
        return out

    def arrived(c, block, part):
        remote(c, 0, block, part, x_peers[0], False).wait_recv()

    late_blocks = [
        lax.rem(my_y + dy, side) * side + lax.rem(my_x + dx, side)
        for dy in range(1, side)
        for dx in range(1, side)
    ]

    def wait_early(c):
        for block in x_peers + y_peers:
            for part in range(2):
                arrived(c, block, part)

    def wait_late(c):
        for block in late_blocks:
            for part in range(2):
                arrived(c, block, part)

    def start_all(copies):
        for copy in copies:
            copy.start()

    start_all(own_copies(0))
    if chunks > 1:
        start_all(own_copies(1))

    small = [
        pltpu.make_async_copy(source, target, local_sem.at[3 + i])
        for i, (source, target) in enumerate((
            (decay_hbm, decay_ref), (inv_hbm, inv_ref), (query_hbm, query_ref),
            (key_hbm, key_ref), (value_hbm, value_ref), (gain_hbm, gain_ref),
        ))
    ]
    for copy in small:
        copy.start()
    local = [
        pltpu.make_async_copy(x_ref, gx.at[me], local_sem.at[0]),
        pltpu.make_async_copy(wk_ref, wk, local_sem.at[1]),
        pltpu.make_async_copy(wv_ref, wv, local_sem.at[2]),
    ]
    for copy in local:
        copy.start()
    state_ref[...] = jnp.zeros_like(state_ref)
    for copy in small:
        copy.wait()
    base = lax.rem(sp_place, seq_span) * tokens

    def table(c, _):
        at = pl.ds(pl.multiple_of(c * half, half), half)
        place = (base + c * half + lax.broadcasted_iota(jnp.int32, (half, width), 0)).astype(F32)
        angle = place * inv_ref[...]
        low = lax.broadcasted_iota(jnp.int32, (half, width), 1) < width // 2
        sin = jnp.sin(angle)
        cosine[at, :] = jnp.cos(angle)
        sine[at, :] = jnp.where(low, -sin, sin)
        return 0

    lax.fori_loop(0, 2 * chunks, table, 0)

    prompt = sp_place // seq_span
    diagonal = lax.broadcasted_iota(jnp.int32, (width, width), 0) == lax.broadcasted_iota(
        jnp.int32, (width, width), 1
    )
    ones = jnp.ones((width, vwidth), BF16)
    queries = query_ref[...].astype(F32)
    next_keys = key_ref[...].astype(F32)
    next_values = value_ref[...].astype(F32)
    for h in range(heads):
        cols = slice(h * width, (h + 1) * width)
        vcols = slice(h * vwidth, (h + 1) * vwidth)
        mine = jnp.zeros((1, width), F32)
        for s in range(SEQS):
            mine = jnp.where(prompt == s, queries[s:s + 1, cols], mine)
            score = jnp.sum(
                queries[s:s + 1, cols] * next_keys[s:s + 1, cols], axis=1, keepdims=True
            )
            own_term[s, h] = score * next_values[s:s + 1, vcols]
        spread = jnp.where(diagonal, jnp.broadcast_to(mine, (width, width)), 0.0).astype(BF16)
        query_wide[h] = jnp.dot(spread, ones, preferred_element_type=F32)
        factor[h] = jnp.exp(jnp.full((1, vwidth), decay_ref[h], F32))

    def state_copies(g):
        piece = pl.ds(g * pair, pair)
        return [
            pltpu.make_async_remote_copy(
                src_ref=staged.at[peer, piece],
                dst_ref=landed.at[sp_place, piece],
                send_sem=state_send.at[g, d],
                recv_sem=state_recv.at[g, sp_place],
                device_id={"sp": peer},
                device_id_type=MESH,
            )
            for d, peer in enumerate(sp_peers)
        ]

    def read_copies():
        return [
            pltpu.make_async_remote_copy(
                src_ref=read,
                dst_ref=reads.at[sp_place],
                send_sem=read_send.at[d],
                recv_sem=read_recv.at[sp_place],
                device_id={"sp": peer},
                device_id_type=MESH,
            )
            for d, peer in enumerate(sp_peers)
        ]

    for copy in local:
        copy.wait()

    def partial(c, blocks, w, cols):
        at = pl.ds(pl.multiple_of(c * rows, rows), rows)
        total = None
        for block in blocks:
            depth = pl.ds(pl.multiple_of(block * feats, feats), feats)
            term = jnp.dot(gx[block, at, :], w[depth, cols], preferred_element_type=F32)
            total = term if total is None else total + term
        return total

    early_blocks = [me] + x_peers + y_peers

    def finish(c, blocks, carry):
        at = pl.ds(pl.multiple_of(c * rows, rows), rows)
        distance = (seq_span * tokens - 1 - base - c * rows) - lax.broadcasted_iota(
            jnp.int32, (rows, width), 0
        )
        distance = distance.astype(F32)

        def step(g, _):
            kcols = pl.ds(pl.multiple_of(g * pair * width, pair * width), pair * width)
            vcols = pl.ds(pl.multiple_of(g * pair * vwidth, pair * vwidth), pair * vwidth)
            k = partial(c, blocks, wk, kcols)
            v = partial(c, blocks, wv, vcols)
            if carry:
                k = k + acc_k[:, kcols]
                v = v + acc_v[:, vcols]
            v = v.astype(BF16)
            for j in range(pair):
                kh = k[:, j * width:(j + 1) * width]
                turned = kh * cosine[at, :] + pltpu.roll(kh, width // 2, 1) * sine[at, :]
                keys = (turned * width ** (-0.5)).astype(BF16).astype(F32)
                weighted = (keys * jnp.exp(decay_ref[g * pair + j] * distance)).astype(BF16)
                state_ref[g * pair + j] += lax.dot_general(
                    weighted, v[:, j * vwidth:(j + 1) * vwidth],
                    (((0,), (0,)), ((), ())), preferred_element_type=F32,
                )
            if carry:
                for j in range(pair):
                    h = g * pair + j
                    held = state_ref[h]
                    for d in range(sp_size):
                        staged[d, h] = held[d * kept:(d + 1) * kept, :].astype(BF16)
                    read[h] = jnp.sum(query_wide[h] * held, axis=0, keepdims=True)
                start_all(state_copies(g))
            return 0

        lax.fori_loop(0, groups, step, 0)

    def round_trip(c, _):
        wait_early(c)
        start_all(relay_copies(c))

        @pl.when(c + 2 < chunks)
        def _():
            start_all(own_copies(c + 2))

        @pl.when(c > 0)
        def _():
            wait_late(c - 1)
            finish(c - 1, early_blocks + late_blocks, False)

        return 0

    lax.fori_loop(0, chunks, round_trip, 0)
    last = chunks - 1

    def early(g, _):
        kcols = pl.ds(pl.multiple_of(g * pair * width, pair * width), pair * width)
        vcols = pl.ds(pl.multiple_of(g * pair * vwidth, pair * vwidth), pair * vwidth)
        acc_k[:, kcols] = partial(last, early_blocks, wk, kcols)
        acc_v[:, vcols] = partial(last, early_blocks, wv, vcols)
        return 0

    lax.fori_loop(0, heads // pair, early, 0)
    wait_late(last)
    finish(last, late_blocks, True)

    start_all(read_copies())
    landed[sp_place] = staged[sp_place]
    reads[sp_place] = read[...]

    for d, peer in enumerate(sp_peers):
        pltpu.make_async_remote_copy(
            src_ref=read, dst_ref=reads.at[peer], send_sem=read_send.at[d],
            recv_sem=read_recv.at[peer], device_id={"sp": peer}, device_id_type=MESH,
        ).wait_recv()
        for g in range(groups):
            piece = pl.ds(g * pair, pair)
            pltpu.make_async_remote_copy(
                src_ref=staged.at[peer, piece], dst_ref=landed.at[peer, piece],
                send_sem=state_send.at[g, d], recv_sem=state_recv.at[g, peer],
                device_id={"sp": peer}, device_id_type=MESH,
            ).wait_recv()

    row = lax.broadcasted_iota(jnp.int32, (SEQS, heads * vwidth), 0)
    out = jnp.zeros((SEQS, heads * vwidth), F32)
    for s in range(SEQS):
        members = range(s * seq_span, (s + 1) * seq_span)
        carried = functools.reduce(jnp.add, [reads[m] for m in members])
        mixed = factor[...] * carried + own_term[s]
        normed = mixed * lax.rsqrt(jnp.mean(mixed * mixed, axis=2, keepdims=True) + 1e-06)
        line = jnp.concatenate([normed[h] for h in range(heads)], axis=1) * gain_ref[...]
        out = jnp.where(row == s, jnp.broadcast_to(line, out.shape), out)
        for h in range(heads):
            cache_ref[s, h] = functools.reduce(
                jnp.add, [landed[m, h].astype(F32) for m in members]
            ).astype(BF16)
    first_ref[...] = out.astype(BF16)

    for copy in read_copies():
        copy.wait_send()
    for g in range(groups):
        for copy in state_copies(g):
            copy.wait_send()

    def drain(c, _):
        for copy in own_copies(c) + relay_copies(c):
            copy.wait_send()
        return 0

    lax.fori_loop(0, chunks, drain, 0)


def settle(cache_ref, first_ref, cache_out, first_out):
    cache_out[...] = cache_ref[...]
    first_out[...] = first_ref[...]


def on_device(
    layer_input, key_weight, value_weight, decay_exponent, query_new, key_new, value_new, norm_gain
):
    tokens, feats = layer_input.shape
    parts = lax.axis_size("tp")
    sp_size = lax.axis_size("sp")
    seq_span = sp_size // SEQS
    side = math.isqrt(parts)
    heads = decay_exponent.shape[0]
    width = key_weight.shape[1] // heads
    vwidth = value_weight.shape[1] // heads
    kept = width // sp_size
    groups = heads // (2 if heads % 2 == 0 else 1)
    steps = np.linspace(0.0, 1.0, width // 2, dtype=np.float32)
    inverse = (np.float32(1.0) / np.power(np.float32(10000.0), steps)).astype(np.float32)
    inverse = jnp.asarray(np.concatenate([inverse, inverse])[None, :])
    sends = 4 * (side - 1) + 2 * (side - 1) ** 2
    anywhere = pl.BlockSpec(memory_space=pl.ANY)
    vmem = pl.BlockSpec(memory_space=pltpu.VMEM)
    rows = tokens // CHUNKS
    state_cache, first_read = pl.pallas_call(
        functools.partial(gather_kernel, side, seq_span, CHUNKS),
        out_shape=(
            jax.ShapeDtypeStruct((SEQS, heads, kept, vwidth), BF16),
            jax.ShapeDtypeStruct((SEQS, heads * vwidth), BF16),
        ),
        in_specs=[anywhere] * 9,
        out_specs=(vmem, vmem),
        scratch_shapes=[
            pltpu.SMEM((heads,), F32),
            pltpu.VMEM(inverse.shape, F32),
            pltpu.VMEM(query_new.shape, BF16),
            pltpu.VMEM(key_new.shape, BF16),
            pltpu.VMEM(value_new.shape, BF16),
            pltpu.VMEM((1, heads * vwidth), F32),
            pltpu.VMEM((parts, tokens, feats), BF16),
            pltpu.VMEM(key_weight.shape, BF16),
            pltpu.VMEM(value_weight.shape, BF16),
            pltpu.VMEM((tokens, width), F32),
            pltpu.VMEM((tokens, width), F32),
            pltpu.VMEM((rows, heads * width), F32),
            pltpu.VMEM((rows, heads * vwidth), F32),
            pltpu.VMEM((heads, width, vwidth), F32),
            pltpu.VMEM((heads, width, vwidth), F32),
            pltpu.VMEM((SEQS, heads, 1, vwidth), F32),
            pltpu.VMEM((heads, 1, vwidth), F32),
            pltpu.VMEM((sp_size, heads, kept, vwidth), BF16),
            pltpu.VMEM((sp_size, heads, kept, vwidth), BF16),
            pltpu.VMEM((heads, 1, vwidth), F32),
            pltpu.VMEM((sp_size, heads, 1, vwidth), F32),
            pltpu.SemaphoreType.DMA((CHUNKS, sends)),
            pltpu.SemaphoreType.DMA((CHUNKS, parts, 2)),
            pltpu.SemaphoreType.DMA((9,)),
            pltpu.SemaphoreType.DMA((groups, sp_size - 1)),
            pltpu.SemaphoreType.DMA((groups, sp_size)),
            pltpu.SemaphoreType.DMA((sp_size - 1,)),
            pltpu.SemaphoreType.DMA((sp_size,)),
        ],
        compiler_params=pltpu.CompilerParams(
            collective_id=0, has_side_effects=True, vmem_limit_bytes=62 * 1024 * 1024
        ),
    )(
        decay_exponent, inverse, query_new, key_new, value_new, norm_gain.reshape(1, -1),
        layer_input, key_weight, value_weight,
    )
    return pl.pallas_call(
        settle,
        out_shape=(
            jax.ShapeDtypeStruct(state_cache.shape, BF16),
            jax.ShapeDtypeStruct(first_read.shape, BF16),
        ),
        in_specs=[vmem, vmem],
        out_specs=(vmem, vmem),
    )(state_cache, first_read)


def solution(mesh):
    in_specs = (
        P("sp", "tp"),
        P(None, "tp"),
        P(None, "tp"),
        P("tp"),
        P(None, "tp"),
        P(None, "tp"),
        P(None, "tp"),
        P("tp"),
    )
    out_specs = (P(None, "tp", "sp", None), P(None, "tp"))
    return jax.shard_map(
        on_device, mesh=mesh, in_specs=in_specs, out_specs=out_specs, check_vma=False
    )
```

```python
import functools
import math

import jax
import jax.numpy as jnp
import numpy as np
from jax import lax
from jax.experimental import pallas as pl
from jax.experimental.pallas import tpu as pltpu
from jax.sharding import PartitionSpec as P

SEQS = 2
CHUNKS = 8
MESH = pl.DeviceIdType.MESH
F32 = jnp.float32
BF16 = jnp.bfloat16


def gather_kernel(
    side, seq_span, chunks,
    decay_hbm, inv_hbm, query_hbm, key_hbm, value_hbm, gain_hbm, x_ref, wk_ref, wv_ref,
    cache_ref, first_ref,
    decay_ref, inv_ref, query_ref, key_ref, value_ref, gain_ref,
    gx, wk, wv, cosine, sine, acc_k, acc_v,
    state_ref, query_wide, own_term, factor, staged, landed, read, reads,
    send_sem, recv_sem, local_sem, state_send, state_recv, read_send, read_recv,
):
    tokens, feats = x_ref.shape
    rows = tokens // chunks
    half = rows // 2
    heads, width, vwidth = state_ref.shape
    pair = next(p for p in (4, 2, 1) if heads % p == 0)
    me = lax.axis_index("tp")
    my_y, my_x = me // side, lax.rem(me, side)
    sp_place = lax.axis_index("sp")
    sp_size = landed.shape[0]
    kept = landed.shape[2]
    groups = heads // pair
    sp_peers = [lax.rem(sp_place + d, sp_size) for d in range(1, sp_size)]

    def x_peer(d):
        return my_y * side + lax.rem(my_x + d, side)

    def y_peer(d):
        return lax.rem(my_y + d, side) * side + my_x

    x_peers = [x_peer(d) for d in range(1, side)]
    y_peers = [y_peer(d) for d in range(1, side)]

    barrier = pltpu.get_barrier_semaphore()
    for peer in x_peers + y_peers:
        pl.semaphore_signal(barrier, inc=1, device_id={"tp": peer}, device_id_type=MESH)
    for peer in sp_peers:
        pl.semaphore_signal(barrier, inc=1, device_id={"sp": peer}, device_id_type=MESH)
    pl.semaphore_wait(barrier, 2 * (side - 1) + sp_size - 1)

    def span(c, part):
        return pl.ds(pl.multiple_of(c * rows + part * half, half), half)

    def remote(c, slot, block, part, target, from_input):
        where = span(c, part)
        return pltpu.make_async_remote_copy(
            src_ref=x_ref.at[where] if from_input else gx.at[block, where],
            dst_ref=gx.at[block, where],
            send_sem=send_sem.at[c, slot],
            recv_sem=recv_sem.at[c, block, part],
            device_id={"tp": target},
            device_id_type=MESH,
        )

    def own_copies(c):
        out, slot = [], 0
        for first in (True, False):
            for part, peers in ((0, x_peers), (1, y_peers)):
                for peer in peers:
                    out.append(remote(c, slot, me, part if first else 1 - part, peer, True))
                    slot += 1
        return out

    def relay_copies(c):
        out, slot = [], 4 * (side - 1)
        for part, sources, peers in ((0, x_peers, y_peers), (1, y_peers, x_peers)):
            for source in sources:
                for peer in peers:
                    out.append(remote(c, slot, source, part, peer, False))
                    slot += 1
        return out

    def arrived(c, block, part):
        remote(c, 0, block, part, x_peers[0], False).wait_recv()

    late_blocks = [
        lax.rem(my_y + dy, side) * side + lax.rem(my_x + dx, side)
        for dy in range(1, side)
        for dx in range(1, side)
    ]

    def wait_early(c):
        for block in x_peers + y_peers:
            for part in range(2):
                arrived(c, block, part)

    def wait_late(c):
        for block in late_blocks:
            for part in range(2):
                arrived(c, block, part)

    def start_all(copies):
        for copy in copies:
            copy.start()

    start_all(own_copies(0))
    if chunks > 1:
        start_all(own_copies(1))

    small = [
        pltpu.make_async_copy(source, target, local_sem.at[3 + i])
        for i, (source, target) in enumerate((
            (decay_hbm, decay_ref), (inv_hbm, inv_ref), (query_hbm, query_ref),
            (key_hbm, key_ref), (value_hbm, value_ref), (gain_hbm, gain_ref),
        ))
    ]
    for copy in small:
        copy.start()
    local = [
        pltpu.make_async_copy(x_ref, gx.at[me], local_sem.at[0]),
        pltpu.make_async_copy(wk_ref, wk, local_sem.at[1]),
        pltpu.make_async_copy(wv_ref, wv, local_sem.at[2]),
    ]
    for copy in local:
        copy.start()
    state_ref[...] = jnp.zeros_like(state_ref)
    for copy in small:
        copy.wait()
    base = lax.rem(sp_place, seq_span) * tokens

    def table(c, _):
        at = pl.ds(pl.multiple_of(c * half, half), half)
        place = (base + c * half + lax.broadcasted_iota(jnp.int32, (half, width), 0)).astype(F32)
        angle = place * inv_ref[...]
        low = lax.broadcasted_iota(jnp.int32, (half, width), 1) < width // 2
        sin = jnp.sin(angle)
        cosine[at, :] = jnp.cos(angle)
        sine[at, :] = jnp.where(low, -sin, sin)
        return 0

    lax.fori_loop(0, 2 * chunks, table, 0)

    prompt = sp_place // seq_span
    diagonal = lax.broadcasted_iota(jnp.int32, (width, width), 0) == lax.broadcasted_iota(
        jnp.int32, (width, width), 1
    )
    ones = jnp.ones((width, vwidth), BF16)
    queries = query_ref[...].astype(F32)
    next_keys = key_ref[...].astype(F32)
    next_values = value_ref[...].astype(F32)
    for h in range(heads):
        cols = slice(h * width, (h + 1) * width)
        vcols = slice(h * vwidth, (h + 1) * vwidth)
        mine = jnp.zeros((1, width), F32)
        for s in range(SEQS):
            mine = jnp.where(prompt == s, queries[s:s + 1, cols], mine)
            score = jnp.sum(
                queries[s:s + 1, cols] * next_keys[s:s + 1, cols], axis=1, keepdims=True
            )
            own_term[s, h] = score * next_values[s:s + 1, vcols]
        spread = jnp.where(diagonal, jnp.broadcast_to(mine, (width, width)), 0.0).astype(BF16)
        query_wide[h] = jnp.dot(spread, ones, preferred_element_type=F32)
        factor[h] = jnp.exp(jnp.full((1, vwidth), decay_ref[h], F32))

    def state_copies(g):
        piece = pl.ds(g * pair, pair)
        return [
            pltpu.make_async_remote_copy(
                src_ref=staged.at[peer, piece],
                dst_ref=landed.at[sp_place, piece],
                send_sem=state_send.at[g, d],
                recv_sem=state_recv.at[g, sp_place],
                device_id={"sp": peer},
                device_id_type=MESH,
            )
            for d, peer in enumerate(sp_peers)
        ]

    def read_copies():
        return [
            pltpu.make_async_remote_copy(
                src_ref=read,
                dst_ref=reads.at[sp_place],
                send_sem=read_send.at[d],
                recv_sem=read_recv.at[sp_place],
                device_id={"sp": peer},
                device_id_type=MESH,
            )
            for d, peer in enumerate(sp_peers)
        ]

    for copy in local:
        copy.wait()

    def partial(c, blocks, w, cols):
        at = pl.ds(pl.multiple_of(c * rows, rows), rows)
        total = None
        for block in blocks:
            depth = pl.ds(pl.multiple_of(block * feats, feats), feats)
            term = jnp.dot(gx[block, at, :], w[depth, cols], preferred_element_type=F32)
            total = term if total is None else total + term
        return total

    early_blocks = [me] + x_peers + y_peers

    def finish(c, blocks, carry):
        at = pl.ds(pl.multiple_of(c * rows, rows), rows)
        distance = (seq_span * tokens - 1 - base - c * rows) - lax.broadcasted_iota(
            jnp.int32, (rows, width), 0
        )
        distance = distance.astype(F32)

        def step(g, _):
            kcols = pl.ds(pl.multiple_of(g * pair * width, pair * width), pair * width)
            vcols = pl.ds(pl.multiple_of(g * pair * vwidth, pair * vwidth), pair * vwidth)
            k = partial(c, blocks, wk, kcols)
            v = partial(c, blocks, wv, vcols)
            if carry:
                k = k + acc_k[:, kcols]
                v = v + acc_v[:, vcols]
            v = v.astype(BF16)
            for j in range(pair):
                kh = k[:, j * width:(j + 1) * width]
                turned = kh * cosine[at, :] + pltpu.roll(kh, width // 2, 1) * sine[at, :]
                keys = (turned * width ** (-0.5)).astype(BF16).astype(F32)
                weighted = (keys * jnp.exp(decay_ref[g * pair + j] * distance)).astype(BF16)
                state_ref[g * pair + j] += lax.dot_general(
                    weighted, v[:, j * vwidth:(j + 1) * vwidth],
                    (((0,), (0,)), ((), ())), preferred_element_type=F32,
                )
            if carry:
                for j in range(pair):
                    h = g * pair + j
                    held = state_ref[h]
                    for d in range(sp_size):
                        staged[d, h] = held[d * kept:(d + 1) * kept, :].astype(BF16)
                    read[h] = jnp.sum(query_wide[h] * held, axis=0, keepdims=True)
                start_all(state_copies(g))
            return 0

        lax.fori_loop(0, groups, step, 0)

    def round_trip(c, _):
        wait_early(c)
        start_all(relay_copies(c))

        @pl.when(c + 2 < chunks)
        def _():
            start_all(own_copies(c + 2))

        @pl.when(c > 0)
        def _():
            wait_late(c - 1)
            finish(c - 1, early_blocks + late_blocks, False)

        return 0

    lax.fori_loop(0, chunks, round_trip, 0)
    last = chunks - 1

    def early(g, _):
        kcols = pl.ds(pl.multiple_of(g * pair * width, pair * width), pair * width)
        vcols = pl.ds(pl.multiple_of(g * pair * vwidth, pair * vwidth), pair * vwidth)
        acc_k[:, kcols] = partial(last, early_blocks, wk, kcols)
        acc_v[:, vcols] = partial(last, early_blocks, wv, vcols)
        return 0

    lax.fori_loop(0, heads // pair, early, 0)
    wait_late(last)
    finish(last, late_blocks, True)

    start_all(read_copies())
    landed[sp_place] = staged[sp_place]
    reads[sp_place] = read[...]

    for d, peer in enumerate(sp_peers):
        pltpu.make_async_remote_copy(
            src_ref=read, dst_ref=reads.at[peer], send_sem=read_send.at[d],
            recv_sem=read_recv.at[peer], device_id={"sp": peer}, device_id_type=MESH,
        ).wait_recv()
        for g in range(groups):
            piece = pl.ds(g * pair, pair)
            pltpu.make_async_remote_copy(
                src_ref=staged.at[peer, piece], dst_ref=landed.at[peer, piece],
                send_sem=state_send.at[g, d], recv_sem=state_recv.at[g, peer],
                device_id={"sp": peer}, device_id_type=MESH,
            ).wait_recv()

    row = lax.broadcasted_iota(jnp.int32, (SEQS, heads * vwidth), 0)
    out = jnp.zeros((SEQS, heads * vwidth), F32)
    for s in range(SEQS):
        members = range(s * seq_span, (s + 1) * seq_span)
        carried = functools.reduce(jnp.add, [reads[m] for m in members])
        mixed = factor[...] * carried + own_term[s]
        normed = mixed * lax.rsqrt(jnp.mean(mixed * mixed, axis=2, keepdims=True) + 1e-06)
        line = jnp.concatenate([normed[h] for h in range(heads)], axis=1) * gain_ref[...]
        out = jnp.where(row == s, jnp.broadcast_to(line, out.shape), out)
        for h in range(heads):
            cache_ref[s, h] = functools.reduce(
                jnp.add, [landed[m, h].astype(F32) for m in members]
            ).astype(BF16)
    first_ref[...] = out.astype(BF16)

    for copy in read_copies():
        copy.wait_send()
    for g in range(groups):
        for copy in state_copies(g):
            copy.wait_send()

    def drain(c, _):
        for copy in own_copies(c) + relay_copies(c):
            copy.wait_send()
        return 0

    lax.fori_loop(0, chunks, drain, 0)


def settle(cache_ref, first_ref, cache_out, first_out):
    cache_out[...] = cache_ref[...]
    first_out[...] = first_ref[...]


def on_device(
    layer_input, key_weight, value_weight, decay_exponent, query_new, key_new, value_new, norm_gain
):
    tokens, feats = layer_input.shape
    parts = lax.axis_size("tp")
    sp_size = lax.axis_size("sp")
    seq_span = sp_size // SEQS
    side = math.isqrt(parts)
    heads = decay_exponent.shape[0]
    width = key_weight.shape[1] // heads
    vwidth = value_weight.shape[1] // heads
    kept = width // sp_size
    groups = heads // next(p for p in (4, 2, 1) if heads % p == 0)
    steps = np.linspace(0.0, 1.0, width // 2, dtype=np.float32)
    inverse = (np.float32(1.0) / np.power(np.float32(10000.0), steps)).astype(np.float32)
    inverse = jnp.asarray(np.concatenate([inverse, inverse])[None, :])
    sends = 4 * (side - 1) + 2 * (side - 1) ** 2
    anywhere = pl.BlockSpec(memory_space=pl.ANY)
    vmem = pl.BlockSpec(memory_space=pltpu.VMEM)
    rows = tokens // CHUNKS
    state_cache, first_read = pl.pallas_call(
        functools.partial(gather_kernel, side, seq_span, CHUNKS),
        out_shape=(
            jax.ShapeDtypeStruct((SEQS, heads, kept, vwidth), BF16),
            jax.ShapeDtypeStruct((SEQS, heads * vwidth), BF16),
        ),
        in_specs=[anywhere] * 9,
        out_specs=(vmem, vmem),
        scratch_shapes=[
            pltpu.SMEM((heads,), F32),
            pltpu.VMEM(inverse.shape, F32),
            pltpu.VMEM(query_new.shape, BF16),
            pltpu.VMEM(key_new.shape, BF16),
            pltpu.VMEM(value_new.shape, BF16),
            pltpu.VMEM((1, heads * vwidth), F32),
            pltpu.VMEM((parts, tokens, feats), BF16),
            pltpu.VMEM(key_weight.shape, BF16),
            pltpu.VMEM(value_weight.shape, BF16),
            pltpu.VMEM((tokens, width), F32),
            pltpu.VMEM((tokens, width), F32),
            pltpu.VMEM((rows, heads * width), F32),
            pltpu.VMEM((rows, heads * vwidth), F32),
            pltpu.VMEM((heads, width, vwidth), F32),
            pltpu.VMEM((heads, width, vwidth), F32),
            pltpu.VMEM((SEQS, heads, 1, vwidth), F32),
            pltpu.VMEM((heads, 1, vwidth), F32),
            pltpu.VMEM((sp_size, heads, kept, vwidth), BF16),
            pltpu.VMEM((sp_size, heads, kept, vwidth), BF16),
            pltpu.VMEM((heads, 1, vwidth), F32),
            pltpu.VMEM((sp_size, heads, 1, vwidth), F32),
            pltpu.SemaphoreType.DMA((CHUNKS, sends)),
            pltpu.SemaphoreType.DMA((CHUNKS, parts, 2)),
            pltpu.SemaphoreType.DMA((9,)),
            pltpu.SemaphoreType.DMA((groups, sp_size - 1)),
            pltpu.SemaphoreType.DMA((groups, sp_size)),
            pltpu.SemaphoreType.DMA((sp_size - 1,)),
            pltpu.SemaphoreType.DMA((sp_size,)),
        ],
        compiler_params=pltpu.CompilerParams(
            collective_id=0, has_side_effects=True, vmem_limit_bytes=62 * 1024 * 1024
        ),
    )(
        decay_exponent, inverse, query_new, key_new, value_new, norm_gain.reshape(1, -1),
        layer_input, key_weight, value_weight,
    )
    return pl.pallas_call(
        settle,
        out_shape=(
            jax.ShapeDtypeStruct(state_cache.shape, BF16),
            jax.ShapeDtypeStruct(first_read.shape, BF16),
        ),
        in_specs=[vmem, vmem],
        out_specs=(vmem, vmem),
    )(state_cache, first_read)


def solution(mesh):
    in_specs = (
        P("sp", "tp"),
        P(None, "tp"),
        P(None, "tp"),
        P("tp"),
        P(None, "tp"),
        P(None, "tp"),
        P(None, "tp"),
        P("tp"),
    )
    out_specs = (P(None, "tp", "sp", None), P(None, "tp"))
    return jax.shard_map(
        on_device, mesh=mesh, in_specs=in_specs, out_specs=out_specs, check_vma=False
    )
```
